32 devices in a mesh: sp: 16 (over z, y, x), tp: 2 (over core).
Axes of the slice: x: 2, y: 2, z: 4, core: 2. Of those that a mesh axis runs over, the one named last changes fastest.
Arguments:
- conv_out: bfloat16 [2048, 2048], P('sp', 'tp'), may hold values from -1500 to 1500
- ln_gain: float32 [2048], P('tp'), may hold values from 0.1 to 1.9
- taps: bfloat16 [31, 2048], P(None, 'tp'), may hold values from -1 to 1
- proj_weight: bfloat16 [2048, 2048], P('sp', 'tp'), may hold values from -0.125 to 0.125
- stream_mid: bfloat16 [2048, 2048], P('sp', 'tp'), may hold values from -6 to 6
- out_grad: bfloat16 [2048, 2048], P('sp', 'tp'), may hold values from -6 to 6
- routes: int32 [2048, 2], P('sp'), may hold values from 0 to 7, all different within a row; in each aligned block of 128 rows (0 to 127, 128 to 255, ...) at most 48 rows name the same one
- route_probs: float32 [2048, 2], P('sp'), may hold values from 0.2 to 1
- gate_slabs: bfloat16 [16, 2048, 1792], P('sp', None, 'tp'), may hold values from -0.125 to 0.125
- up_slabs: bfloat16 [16, 2048, 1792], P('sp', None, 'tp'), may hold values from -0.125 to 0.125
- down_slabs: bfloat16 [16, 1792, 2048], P('sp', 'tp'), may hold values from -0.09375 to 0.09375
Outputs:
- grad_input: bfloat16 [2048, 2048], P('sp', 'tp')
- grad_proj: float32 [2048, 2048], P('sp', 'tp')
- grad_gate: bfloat16 [16, 2048, 1792], P('sp', None, 'tp')
- grad_up: bfloat16 [16, 2048, 1792], P('sp', None, 'tp')
- grad_down: bfloat16 [16, 1792, 2048], P('sp', 'tp')
The draws below stay inside these ranges and needn't reach their ends.
Inputs may be any that keep to these rules, and one draw needn't show every extreme that they name: `routes`: each row names two different experts. Among the rows of one device no expert is named more than 48 times, and in every draw some device's rows name some expert exactly 48 times.
All inputs are finite; a program needn't handle non-finite values.
Results may differ from the reference program's by a relative error of at most 0.015.
Values may be sent and summed in bfloat16 or wider, within the bound.
No kernel may reach another device: no remote copies, remote signals or barrier semaphores. Data moves between devices by JAX's collectives and lax.ppermute only.
A program may use at most 128 MiB of HBM per device.

```python
import math
import jax
import jax.numpy as jnp
import numpy as np
from jax import lax

D = 2048
EXP_HIDDEN = 3584
CONV_WIDTH = 31
TOK_DEV = 128
EXPERTS = 8
CAP = 48
TOKENS = 2048
N_SP = 16
N_TP = 2


def draw_conv_out(key, part):
    keys = jax.random.split(key, 3)
    columns = jnp.arange(D, dtype=jnp.float32)
    col_scale = jnp.exp(jax.random.uniform(keys[0], (D,), jnp.float32, 0.0, math.log(10.0))) * 3.0 ** (columns / D)
    row_scale = jnp.exp(jax.random.uniform(keys[1], (TOKENS, 1), jnp.float32, 0.0, math.log(10.0)))
    base = jnp.clip(jax.random.normal(keys[2], (TOKENS, D), jnp.float32), -5.0, 5.0)
    return (base * col_scale[None, :] * row_scale).astype(jnp.bfloat16)


def with_spikes(array, stream_key, source, target, parts, factor):
    owner, partner = [(jnp.arange(array.shape[axis_at]) // (array.shape[axis_at] // parts)).reshape([-1 if axis == axis_at else 1 for axis in range(array.ndim)]) for axis_at in (source, target)]
    chosen = jax.random.permutation(stream_key, parts)[partner]
    strong = (owner == chosen) | (owner == (partner + parts // 2) % parts)
    return jnp.where(strong, factor * array, array)


def steps_of(key, shape, shards, low, top_value):
    def one(dim, parts):
        draws = jax.random.uniform(jax.random.fold_in(jax.random.fold_in(key, 6), dim), (parts,), jnp.float32, low / len(shards), top_value / len(shards))
        return jnp.repeat(jnp.exp(draws), shape[dim] // parts).reshape((-1,) + (1,) * (len(shape) - dim - 1))

    loudness = one(*shards[0])
    for cut in shards[1:]:
        loudness = loudness * one(*cut)
    return loudness


def shared_out(own_key, own, number, rows, amount, top, most, skew):
    sequence = jax.random.permutation(own_key, amount)
    crowded, common = load_shares(amount, rows * top, most, skew, True), load_shares(amount, rows * top, most, skew, False)
    places = jnp.arange(amount)

    def named(tallies, offset_by):
        used = int((tallies > 0).sum())
        fixed = max(1, used // 4)
        passed = fixed + (places - fixed + offset_by * (used - fixed)) % max(1, amount - fixed)
        return jnp.zeros((amount,), jnp.int32).at[sequence[jnp.where(places < fixed, places, passed)]].set(jnp.asarray(tallies, jnp.int32))

    tallies = jnp.where(number % 4 == 0, named(crowded, number // 4), named(common, number - number // 4 - 1))
    mixed = jax.random.permutation(jax.random.fold_in(own, 3), amount)
    source_of, receiver = mixed[0:amount // 2 * 2:2], mixed[1:amount // 2 * 2:2]
    margin = jnp.minimum(tallies[source_of] - 1, most - tallies[receiver]) // 2
    margin = jnp.where((source_of == sequence[0]) | (receiver == sequence[0]) | (tallies[receiver] == 0), 0, jnp.maximum(margin, 0))
    passed = jax.random.randint(jax.random.fold_in(own, 4), (amount // 2,), 0, 1 << 20) % (margin + 1)
    tallies = tallies.at[source_of].add(-passed).at[receiver].add(passed)
    items = jnp.searchsorted(jnp.cumsum(tallies), jnp.arange(rows * top), side="right").astype(jnp.int32)
    table = items.reshape(top, rows).T
    table = table[jax.random.permutation(jax.random.fold_in(own, 1), rows)]
    offset_by = jax.random.randint(jax.random.fold_in(own, 2), (rows, 1), 0, top)
    return jnp.take_along_axis(table, (jnp.arange(top)[None, :] + offset_by) % top, axis=1)


def load_shares(count, total, bound, skew, full):
    weights = [(1 << 20) // math.isqrt(grade ** skew) + 1 for grade in range(1, count + 1)]
    largest = bound if full else min(bound, max(-(-total // count), total * weights[0] // sum(weights)))
    least = 1 if total - largest >= count - 1 else 0
    given, rest = [largest] + [least] * (count - 1), total - largest - least * (count - 1)
    while rest > 0:
        free = [i for i in range(1, count) if given[i] < largest] or [i for i in range(1, count) if given[i] < bound]
        pool, left = sum([weights[i] for i in free]), rest
        for i in free:
            more = min(bound - given[i], max(1, left * weights[i] // pool), rest)
            given[i] = given[i] + more
            rest = rest - more
    return np.array(given)


def scatter_about(key, extent, deviation, most, pieces=(), kind=jnp.bfloat16):
    array = deviation * jax.random.normal(key, extent, jnp.float32)
    if pieces:
        array = array * steps_of(key, extent, pieces, -0.22, 0.18)
    return jnp.clip(array, -most, most).astype(kind)


def gaussian_with(key, shape, width, most, shards, heavy, kind=jnp.bfloat16):
    values = width * jax.random.normal(key, shape, jnp.float32)
    if shards:
        values = values * steps_of(key, shape, shards, -0.22, 0.18)
    return jnp.clip(with_spikes(values, jax.random.fold_in(key, 3), *heavy), -most, most).astype(kind)


def setup_inputs(seed: int = 0) -> dict:
    splits = jax.random.split(jax.random.key(seed), 12)
    conv_out = draw_conv_out(jax.random.fold_in(splits[11], 71), 0)
    ln_gain = jnp.clip(1.0 + 0.18 * jax.random.normal(splits[1], (D,), jnp.float32), 0.1, 1.9)
    taps = scatter_about(splits[2], (CONV_WIDTH, D), CONV_WIDTH ** -0.5, 1.0, ((1, 2),))
    proj_weight = scatter_about(splits[3], (D, D), D ** -0.5, 0.125, ((0, 16), (1, 2)))
    stream_mid = scatter_about(splits[4], (TOKENS, D), 1.0, 6.0, ((0, 16), (1, 2)))
    out_grad = gaussian_with(splits[5], (TOKENS, D), 1.0, 6.0, ((0, 16), (1, 2)), (0, 1, 16, 2.0))
    routes_keys = jax.random.split(jax.random.fold_in(splits[6], 1), TOKENS // TOK_DEV)
    routes_turns = jax.random.permutation(jax.random.fold_in(splits[6], 3), TOKENS // TOK_DEV)
    routes = jax.vmap(lambda own, number: shared_out(jax.random.fold_in(splits[6], 2), own, number, TOK_DEV, EXPERTS, 2, CAP, 1))(routes_keys, routes_turns).reshape((TOKENS, 2))
    route_probs = jnp.clip(0.2 + 0.8 * jax.random.uniform(splits[7], (TOKENS, 2), jnp.float32) ** steps_of(splits[7], (TOKENS, 2), ((0, 16),), -0.2, 0.2), 0.2, 1.0)
    gate_slabs = scatter_about(splits[8], (2 * EXPERTS, D, EXP_HIDDEN // 2), D ** -0.5, 0.125, ((0, 16), (2, 2)))
    up_slabs = scatter_about(splits[9], (2 * EXPERTS, D, EXP_HIDDEN // 2), D ** -0.5, 0.125, ((0, 16), (2, 2)))
    down_slabs = scatter_about(splits[10], (2 * EXPERTS, EXP_HIDDEN // 2, D), EXP_HIDDEN ** -0.5, 0.09375, ((0, 16), (1, 2)))
    return {"conv_out": conv_out, "ln_gain": ln_gain, "taps": taps, "proj_weight": proj_weight, "stream_mid": stream_mid, "out_grad": out_grad, "routes": routes, "route_probs": route_probs, "gate_slabs": gate_slabs, "up_slabs": up_slabs, "down_slabs": down_slabs}


def dispatch_table(route_block, experts, capacity):
    tok_rows = route_block.shape[0]
    labels = jnp.arange(experts, dtype=jnp.int32)
    onehot = (route_block[:, :, None] == labels[None, None, :]).astype(jnp.float32)
    per_token = lax.optimization_barrier(jnp.sum(onehot, axis=1))
    earlier = (jnp.arange(tok_rows)[:, None] > jnp.arange(tok_rows)[None, :]).astype(jnp.float32)
    before = jnp.dot(earlier, per_token, precision=lax.Precision.HIGHEST)
    slot_index = lax.optimization_barrier(jnp.sum(onehot * before[:, None, :], axis=2)).astype(jnp.int32)
    position = route_block * capacity + slot_index
    columns = jnp.arange(experts * capacity, dtype=jnp.int32)
    first_pick = position[:, 0:1] == columns[None, :]
    second_pick = position[:, 1:2] == columns[None, :]
    return (first_pick, second_pick)

def half_grads(expert_in, expert_grad, weight, w_gate, w_up, w_down):
    gate_value = jnp.dot(expert_in, w_gate, preferred_element_type=jnp.float32)
    up_value = jnp.dot(expert_in, w_up, preferred_element_type=jnp.float32)
    gate_sig = jax.nn.sigmoid(gate_value)
    hidden_act = gate_value * gate_sig * up_value
    scaled = (weight[:, None] * hidden_act).astype(jnp.bfloat16)
    grad_down = jnp.dot(scaled.T, expert_grad, preferred_element_type=jnp.float32).astype(jnp.bfloat16)
    grad_hidden = weight[:, None] * jnp.dot(expert_grad, w_down.T, preferred_element_type=jnp.float32)
    grad_gate_pre = (grad_hidden * up_value * gate_sig * (1.0 + gate_value * (1.0 - gate_sig))).astype(jnp.bfloat16)
    grad_up_pre = (grad_hidden * gate_value * gate_sig).astype(jnp.bfloat16)
    grad_gate = jnp.dot(expert_in.T, grad_gate_pre, preferred_element_type=jnp.float32).astype(jnp.bfloat16)
    grad_up = jnp.dot(expert_in.T, grad_up_pre, preferred_element_type=jnp.float32).astype(jnp.bfloat16)
    quarter = w_gate.shape[1] // N_TP
    returned = jnp.zeros(expert_in.shape, jnp.float32)
    for core_index in range(N_TP):
        low_col = core_index * quarter
        high_col = low_col + quarter
        piece = jnp.dot(grad_gate_pre[:, low_col:high_col], w_gate[:, low_col:high_col].T, preferred_element_type=jnp.float32)
        piece = piece + jnp.dot(grad_up_pre[:, low_col:high_col], w_up[:, low_col:high_col].T, preferred_element_type=jnp.float32)
        rounded = lax.optimization_barrier(piece.astype(jnp.bfloat16))
        returned = returned + rounded.astype(jnp.float32)
    return (grad_gate, grad_up, grad_down, returned.astype(jnp.bfloat16))

def reference(conv_out, ln_gain, taps, proj_weight, stream_mid, out_grad, routes, route_probs, gate_slabs, up_slabs, down_slabs):
    slot_count = EXPERTS * CAP
    half_width = EXP_HIDDEN // 2

    def pack(inputs):
        route_block, mid_block, grad_block, prob_block = inputs
        first_pick, second_pick = dispatch_table(route_block, EXPERTS, CAP)
        route_table = (first_pick | second_pick).astype(jnp.float32)
        mid_slots = jnp.dot(route_table.T, mid_block.astype(jnp.float32), precision=lax.Precision.HIGHEST).astype(jnp.bfloat16)
        grad_slots = jnp.dot(route_table.T, grad_block.astype(jnp.float32), precision=lax.Precision.HIGHEST).astype(jnp.bfloat16)
        prob_slots = lax.optimization_barrier(jnp.sum(first_pick.astype(jnp.float32) * prob_block[:, 0:1] + second_pick.astype(jnp.float32) * prob_block[:, 1:2], axis=0))
        return (mid_slots, grad_slots, prob_slots)
    mid_slots, grad_slots, prob_slots = lax.map(pack, (routes.reshape(N_SP, TOK_DEV, 2), stream_mid.reshape(N_SP, TOK_DEV, D), out_grad.reshape(N_SP, TOK_DEV, D), route_probs.reshape(N_SP, TOK_DEV, 2)))

    def by_expert(slots):
        return slots.reshape(N_SP, EXPERTS, CAP, D).transpose(1, 0, 2, 3).reshape(EXPERTS, N_SP * CAP, D)
    probs_expert = prob_slots.reshape(N_SP, EXPERTS, CAP).transpose(1, 0, 2).reshape(EXPERTS, N_SP * CAP)

    def expert(inputs):
        expert_in, expert_grad, weight, gates, ups, downs = inputs
        first_half = half_grads(expert_in, expert_grad, weight, gates[0], ups[0], downs[0])
        second_half = half_grads(expert_in, expert_grad, weight, gates[1], ups[1], downs[1])
        return (jnp.stack([first_half[0], second_half[0]]), jnp.stack([first_half[1], second_half[1]]), jnp.stack([first_half[2], second_half[2]]), jnp.stack([first_half[3], second_half[3]]))
    grad_gate, grad_up, grad_down, returned = lax.map(expert, (by_expert(mid_slots), by_expert(grad_slots), probs_expert, gate_slabs.reshape(EXPERTS, 2, D, half_width), up_slabs.reshape(EXPERTS, 2, D, half_width), down_slabs.reshape(EXPERTS, 2, half_width, D)))
    returned = returned.reshape(EXPERTS, 2, N_SP, CAP, D).transpose(2, 0, 1, 3, 4)

    def unpack(inputs):
        route_block, back_rows, grad_block = inputs
        first_pick, second_pick = dispatch_table(route_block, EXPERTS, CAP)
        route_table = (first_pick | second_pick).astype(jnp.bfloat16)
        contrib = jnp.dot(route_table, back_rows[:, 0].reshape(slot_count, D), preferred_element_type=jnp.float32)
        contrib = contrib + jnp.dot(route_table, back_rows[:, 1].reshape(slot_count, D), preferred_element_type=jnp.float32)
        return (grad_block.astype(jnp.float32) + contrib).astype(jnp.bfloat16)
    grad_stream = lax.map(unpack, (routes.reshape(N_SP, TOK_DEV, 2), returned, out_grad.reshape(N_SP, TOK_DEV, D))).reshape(TOKENS, D)
    values = conv_out.astype(jnp.float32)
    row_mean = lax.optimization_barrier(jnp.mean(values, axis=1, keepdims=True))
    row_var = lax.optimization_barrier(jnp.mean(values * values, axis=1, keepdims=True)) - row_mean * row_mean
    inv_std = lax.rsqrt(row_var + 1e-06)
    normed = (values - row_mean) * inv_std
    scaled_z = normed * ln_gain[None, :]
    z_sig = jax.nn.sigmoid(scaled_z)
    activated = (scaled_z * z_sig).astype(jnp.bfloat16)
    grad_act = jnp.dot(grad_stream, proj_weight, preferred_element_type=jnp.float32)
    grad_normed = grad_act * z_sig * (1.0 + scaled_z * (1.0 - z_sig)) * ln_gain[None, :]
    first_mean = lax.optimization_barrier(jnp.mean(grad_normed, axis=1, keepdims=True))
    second_mean = lax.optimization_barrier(jnp.mean(grad_normed * normed, axis=1, keepdims=True))
    grad_conv = (inv_std * (grad_normed - first_mean - normed * second_mean)).astype(jnp.bfloat16)
    extended = jnp.concatenate([grad_conv, jnp.zeros((CONV_WIDTH - 1, D), jnp.bfloat16)], axis=0).astype(jnp.float32)
    tap_values = taps.astype(jnp.float32)
    grad_input = jnp.zeros((TOKENS, D), jnp.float32)
    for offset in range(CONV_WIDTH):
        grad_input = grad_input + tap_values[offset][None, :] * extended[offset:offset + TOKENS]
    grad_proj = jnp.dot(grad_stream.T, activated, preferred_element_type=jnp.float32)
    return (grad_input.astype(jnp.bfloat16), grad_proj, grad_gate.reshape(2 * EXPERTS, D, half_width), grad_up.reshape(2 * EXPERTS, D, half_width), grad_down.reshape(2 * EXPERTS, half_width, D))
```

```python
import jax
import jax.numpy as jnp
from jax import lax
from jax.sharding import Mesh
from jax.sharding import PartitionSpec as P


SP = ("far", "side", "pair")
fence = lax.optimization_barrier


def swapped(value, axis):
    return lax.ppermute(value, axis, [(0, 1), (1, 0)])


def shifted(value, steps):
    count = lax.axis_size("far")
    return lax.ppermute(value, "far", [(s, (s + steps) % count) for s in range(count)])


def passed_along(value, steps):
    count = lax.axis_size(SP)
    first, last = (max(0, -steps), min(count, count - steps))
    return lax.ppermute(value, SP, [(source, source + steps) for source in range(first, last)])


def chosen(bit, low, high):
    return jnp.where(bit == 0, low, high)


def slot_columns(info, targets, capacity):
    rows = info.shape[1]
    routes = info[0:2]
    probs = info[2:4]
    wide = targets.shape[0] * capacity
    earlier = (jnp.arange(rows)[:, None] > jnp.arange(rows)[None, :]).astype(jnp.bfloat16)
    target_of = jnp.repeat(targets, capacity).astype(jnp.float32)
    slot_of = (jnp.arange(wide) % capacity).astype(jnp.float32)
    first = routes[0][:, None] == target_of[None, :]
    second = routes[1][:, None] == target_of[None, :]
    named = (first | second).astype(jnp.bfloat16)
    before = jnp.dot(earlier, named, preferred_element_type=jnp.float32)
    here = before == slot_of[None, :]
    first, second = (first & here, second & here)
    weights = jnp.sum(
        jnp.where(first, probs[0][:, None], 0.0) + jnp.where(second, probs[1][:, None], 0.0),
        axis=0,
    )
    return ((first | second).astype(jnp.bfloat16), weights)


def contract_rows(left, right):
    return lax.dot_general(
        left, right, (((0,), (0,)), ((), ())), preferred_element_type=jnp.float32
    )


def contract_cols(left, right):
    return lax.dot_general(
        left, right, (((1,), (1,)), ((), ())), preferred_element_type=jnp.float32
    )


def on_device(
    conv_out,
    ln_gain,
    taps,
    proj_weight,
    stream_mid,
    out_grad,
    routes,
    route_probs,
    gate_slabs,
    up_slabs,
    down_slabs,
):
    tok_rows, half = conv_out.shape
    width = half * lax.axis_size("tp")
    planes = lax.axis_size("far")
    experts = 2 * planes
    capacity = 3 * tok_rows // experts
    out_rows = proj_weight.shape[0]
    core = lax.axis_index("tp")
    plane = lax.axis_index("far")
    side = lax.axis_index("side")
    pair = lax.axis_index("pair")
    wide = planes * capacity
    hops = range(1, planes)

    info = jnp.concatenate([routes.astype(jnp.float32).T, route_probs.T], axis=0)
    beside_info = swapped(info, "side")
    beside_mid = swapped(stream_mid, "side")
    beside_grad = swapped(out_grad, "side")

    values = conv_out.astype(jnp.float32)
    row_total, row_squares = lax.psum(
        (jnp.sum(values, axis=1), jnp.sum(values * values, axis=1)), "tp"
    )
    row_mean = row_total[:, None] / width
    row_var = row_squares[:, None] / width - row_mean * row_mean
    inv_std = lax.rsqrt(row_var + 1e-06)
    normed = (values - row_mean) * inv_std
    scaled_z = normed * ln_gain[None, :]
    z_sig = jax.nn.sigmoid(scaled_z)
    activated = (scaled_z * z_sig).astype(jnp.bfloat16)

    targets = 2 * ((plane + jnp.arange(planes)) % planes) + side
    own_table, own_weights = slot_columns(info, targets, capacity)
    beside_table, beside_weights = slot_columns(beside_info, targets, capacity)

    def by_target(near, far):
        near, far = (
            block.astype(jnp.bfloat16).reshape(planes, capacity, half) for block in (near, far)
        )
        return [jnp.stack([near[k], far[k]]) for k in range(planes)]

    mid_slots = by_target(
        contract_rows(own_table, stream_mid), contract_rows(beside_table, beside_mid)
    )
    grad_slots = by_target(
        contract_rows(own_table, out_grad) * own_weights[:, None],
        contract_rows(beside_table, beside_grad) * beside_weights[:, None],
    )
    mid_far = [shifted(mid_slots[k], k) for k in hops]
    mid_far, grad_slots, activated = fence((mid_far, grad_slots, activated))
    mid_mine = jnp.stack([mid_slots[0], *mid_far]).reshape(2 * wide, half)
    mid_pair = swapped(mid_mine, "pair")
    grad_far = [shifted(grad_slots[k], k) for k in hops]
    mid_pair, grad_far, proj_held, act_held = fence(
        (mid_pair, grad_far, proj_weight, activated)
    )
    grad_mine = jnp.stack([grad_slots[0], *grad_far]).reshape(2 * wide, half)
    grad_pair = swapped(grad_mine, "pair")
    proj_far = [shifted(proj_held, k) for k in hops]
    act_far = [shifted(act_held, k) for k in hops]

    def assembled(mine, paired):
        rows = jnp.concatenate([mine, paired], axis=0)
        other = swapped(rows, "tp")
        return chosen(
            core,
            jnp.concatenate([rows, other], axis=1),
            jnp.concatenate([other, rows], axis=1),
        )

    def in_order(own, pieces):
        held = jnp.zeros((planes, *own.shape), own.dtype)
        for k, piece in enumerate([own, *pieces]):
            held = lax.dynamic_update_slice(
                held, piece[None], ((plane - k) % planes,) + (0,) * own.ndim
            )
        return held.reshape(planes * own.shape[0], own.shape[1])

    expert_in = fence(assembled(mid_mine, mid_pair))
    expert_grad = fence(assembled(grad_mine, grad_pair))
    w_gate = gate_slabs[0]
    w_up = up_slabs[0]
    w_down = down_slabs[0]
    gate_value = jnp.dot(expert_in, w_gate, preferred_element_type=jnp.float32)
    up_value = jnp.dot(expert_in, w_up, preferred_element_type=jnp.float32)
    gate_sig = jax.nn.sigmoid(gate_value)
    hidden_act = (gate_value * gate_sig * up_value).astype(jnp.bfloat16)
    grad_hidden = contract_cols(expert_grad, w_down)
    grad_gate_pre = (
        grad_hidden * up_value * gate_sig * (1.0 + gate_value * (1.0 - gate_sig))
    ).astype(jnp.bfloat16)
    grad_up_pre = (grad_hidden * gate_value * gate_sig).astype(jnp.bfloat16)
    partial_value = (
        contract_cols(grad_gate_pre, w_gate) + contract_cols(grad_up_pre, w_up)
    ).astype(jnp.bfloat16)
    low, high = (partial_value[:, :half], partial_value[:, half:])
    given = swapped(chosen(core, high, low), "tp")
    summed = (chosen(core, low, high).astype(jnp.float32) + given.astype(jnp.float32)).astype(
        jnp.bfloat16
    )
    proj_mine = in_order(proj_weight, proj_far)
    proj_side = swapped(proj_mine, "side")
    act_mine = in_order(activated, act_far)
    act_side = swapped(act_mine, "side")
    across = swapped(summed[2 * wide :], "pair")
    both = (summed[: 2 * wide].astype(jnp.float32) + across.astype(jnp.float32)).astype(
        jnp.bfloat16
    )
    both = both.reshape(planes, 2, capacity, half)
    back = jnp.stack([both[0]] + [shifted(both[k], -k) for k in hops])
    for_beside = jnp.dot(
        beside_table, back[:, 1].reshape(wide, half), preferred_element_type=jnp.float32
    ).astype(jnp.bfloat16)
    for_own = jnp.dot(
        own_table, back[:, 0].reshape(wide, half), preferred_element_type=jnp.float32
    )
    from_beside = swapped(for_beside, "side")
    grad_stream = (
        out_grad.astype(jnp.float32) + for_own + from_beside.astype(jnp.float32)
    ).astype(jnp.bfloat16)

    grad_down = contract_rows(hidden_act, expert_grad).astype(jnp.bfloat16)
    grad_gate = contract_rows(expert_in, grad_gate_pre).astype(jnp.bfloat16)
    grad_up = contract_rows(expert_in, grad_up_pre).astype(jnp.bfloat16)

    by_pair = grad_stream.reshape(tok_rows, half // (2 * out_rows), 2, out_rows)
    even, odd = (by_pair[:, :, 0].reshape(tok_rows, -1), by_pair[:, :, 1].reshape(tok_rows, -1))
    stream_kept = chosen(pair, even, odd)
    stream_met = swapped(chosen(pair, odd, even), "pair")
    shared = lax.all_gather(
        jnp.concatenate([stream_kept, stream_met], axis=0), "tp", axis=1, tiled=True
    )
    shared = shared.reshape(2 * tok_rows, planes, 2, out_rows)
    side_cols = [shared[:, :, s].reshape(2 * tok_rows, planes * out_rows) for s in range(2)]
    near_cols = chosen(side, side_cols[0], side_cols[1])
    far_cols = chosen(side, side_cols[1], side_cols[0])
    act_partial = jnp.dot(near_cols, proj_mine, preferred_element_type=jnp.float32) + jnp.dot(
        far_cols, proj_side, preferred_element_type=jnp.float32
    )
    act_met = swapped(act_partial[tok_rows:].astype(jnp.bfloat16), "pair")
    grad_act = act_partial[:tok_rows] + act_met.astype(jnp.float32)

    whole_stream = lax.all_gather(grad_stream, "tp", axis=1, tiled=True)
    own_columns = lax.all_to_all(
        whole_stream, ("far", "side"), split_axis=1, concat_axis=0, tiled=True
    )
    grad_normed = grad_act * z_sig * (1.0 + scaled_z * (1.0 - z_sig)) * ln_gain[None, :]
    first_sum, second_sum = lax.psum(
        (jnp.sum(grad_normed, axis=1), jnp.sum(grad_normed * normed, axis=1)), "tp"
    )
    grad_conv = (
        inv_std * (grad_normed - first_sum[:, None] / width - normed * second_sum[:, None] / width)
    ).astype(jnp.bfloat16)
    reach_rows = taps.shape[0] - 1
    following = passed_along(grad_conv[:reach_rows], -1)
    extended = jnp.concatenate([grad_conv, following], axis=0).astype(jnp.float32)
    tap_values = taps.astype(jnp.float32)
    grad_input = jnp.zeros((tok_rows, grad_conv.shape[1]), jnp.float32)
    for offset in range(taps.shape[0]):
        grad_input = grad_input + tap_values[offset][None, :] * extended[offset : offset + tok_rows]

    columns = own_columns.reshape(planes, 2, tok_rows, 2 * out_rows)
    near_rows = chosen(side, columns[:, 0], columns[:, 1]).reshape(planes * tok_rows, 2 * out_rows)
    far_rows = chosen(side, columns[:, 1], columns[:, 0]).reshape(planes * tok_rows, 2 * out_rows)
    proj_partial = contract_rows(near_rows, act_mine) + contract_rows(far_rows, act_side)
    first_rows, second_rows = (proj_partial[:out_rows], proj_partial[out_rows:])
    proj_met = swapped(chosen(pair, second_rows, first_rows).astype(jnp.bfloat16), "pair")
    grad_proj = chosen(pair, first_rows, second_rows) + proj_met.astype(jnp.float32)
    return (
        grad_input.astype(jnp.bfloat16),
        grad_proj,
        grad_gate[None],
        grad_up[None],
        grad_down[None],
    )


def solution(mesh):
    places, cores = mesh.devices.shape
    split = Mesh(mesh.devices.reshape(places // 4, 2, 2, cores), (*SP, "tp"))
    return jax.shard_map(
        on_device,
        mesh=split,
        in_specs=(
            P(SP, "tp"),
            P("tp"),
            P(None, "tp"),
            P(SP, "tp"),
            P(SP, "tp"),
            P(SP, "tp"),
            P(SP, None),
            P(SP, None),
            P(SP, None, "tp"),
            P(SP, None, "tp"),
            P(SP, "tp", None),
        ),
        out_specs=(
            P(SP, "tp"),
            P(SP, "tp"),
            P(SP, None, "tp"),
            P(SP, None, "tp"),
            P(SP, "tp", None),
        ),
        check_vma=False,
    )
```

```python
import functools

import jax
import jax.numpy as jnp
from jax import lax
from jax.experimental import pallas as pl
from jax.experimental.pallas import tpu as pltpu
from jax.sharding import Mesh
from jax.sharding import PartitionSpec as P


SP = ("far", "side", "pair")
fence = lax.optimization_barrier


def swapped(value, axis):
    return lax.ppermute(value, axis, [(0, 1), (1, 0)])


def shifted(value, steps):
    count = lax.axis_size("far")
    return lax.ppermute(value, "far", [(s, (s + steps) % count) for s in range(count)])


def passed_along(value, steps):
    count = lax.axis_size(SP)
    first, last = (max(0, -steps), min(count, count - steps))
    return lax.ppermute(value, SP, [(source, source + steps) for source in range(first, last)])


def chosen(bit, low, high):
    return jnp.where(bit == 0, low, high)


def slot_columns(info, targets, capacity):
    rows = info.shape[1]
    routes = info[0:2]
    probs = info[2:4]
    wide = targets.shape[0] * capacity
    earlier = (jnp.arange(rows)[:, None] > jnp.arange(rows)[None, :]).astype(jnp.bfloat16)
    target_of = jnp.repeat(targets, capacity).astype(jnp.float32)
    slot_of = (jnp.arange(wide) % capacity).astype(jnp.float32)
    first = routes[0][:, None] == target_of[None, :]
    second = routes[1][:, None] == target_of[None, :]
    named = (first | second).astype(jnp.bfloat16)
    before = jnp.dot(earlier, named, preferred_element_type=jnp.float32)
    here = before == slot_of[None, :]
    first, second = (first & here, second & here)
    weights = jnp.sum(
        jnp.where(first, probs[0][:, None], 0.0) + jnp.where(second, probs[1][:, None], 0.0),
        axis=0,
    )
    return ((first | second).astype(jnp.bfloat16), weights)


def contract_rows(left, right):
    return lax.dot_general(
        left, right, (((0,), (0,)), ((), ())), preferred_element_type=jnp.float32
    )


def contract_cols(left, right):
    return lax.dot_general(
        left, right, (((1,), (1,)), ((), ())), preferred_element_type=jnp.float32
    )


def own_and_other(half):
    core = lax.axis_index("tp")
    own = pl.ds(pl.multiple_of(core * half, half), half)
    other = pl.ds(pl.multiple_of((1 - core) * half, half), half)
    return (own, other)


def dotted(left, right):
    return jnp.dot(left, right, preferred_element_type=jnp.float32)


def in_vmem(kernel, shapes, flops, arrays, scratch=(), limit=24):
    return pl.pallas_call(
        kernel,
        out_shape=shapes,
        in_specs=[pl.BlockSpec(memory_space=pltpu.VMEM)] * len(arrays),
        out_specs=jax.tree.map(lambda _: pl.BlockSpec(memory_space=pltpu.VMEM), shapes),
        scratch_shapes=[pltpu.VMEM(shape, dtype) for shape, dtype in scratch],
        cost_estimate=pl.CostEstimate(
            flops=flops, bytes_accessed=sum(a.size * 2 for a in arrays), transcendentals=0
        ),
        compiler_params=pltpu.CompilerParams(vmem_limit_bytes=limit << 20),
    )(*arrays)


LANES = 128


def gathered(pieces, held):
    half = held.shape[1] // 2
    count = len(pieces) // 2
    for column, group in enumerate((pieces[:count], pieces[count:])):
        start = 0
        for piece in group:
            rows = piece.shape[0]
            held[start : start + rows, column * half : (column + 1) * half] = piece[...]
            start += rows


def hidden_kernel(*refs):
    pieces = refs[:8]
    gate_w, up_w, act_ref, gate_f, up_f, held = refs[8:]
    own, other = own_and_other(held.shape[1] // 2)
    gathered(pieces, held)

    def step(i, carry):
        cols = pl.ds(pl.multiple_of(i * LANES, LANES), LANES)
        own_w = jnp.concatenate([gate_w[0, own, cols], up_w[0, own, cols]], axis=1)
        oth_w = jnp.concatenate([gate_w[0, other, cols], up_w[0, other, cols]], axis=1)
        both = dotted(held[...], jnp.concatenate([own_w, oth_w], axis=0))
        gate, up = (both[:, :LANES], both[:, LANES:])
        sig = jax.nn.sigmoid(gate)
        silu = gate * sig
        act_ref[:, cols] = (silu * up).astype(act_ref.dtype)
        gate_f[:, cols] = (up * sig * (1.0 + gate * (1.0 - sig))).astype(gate_f.dtype)
        up_f[:, cols] = silu.astype(up_f.dtype)
        return carry

    lax.fori_loop(0, gate_w.shape[2] // LANES, step, 0)


def pre_kernel(*refs):
    pieces = refs[:8]
    down_w, gate_f, up_f, gate_pre, up_pre, held = refs[8:]
    own, other = own_and_other(held.shape[1] // 2)
    count = down_w.shape[1]
    gathered(pieces, held)

    def piece(start, size):
        at_w = pl.ds(start, size)
        weights = jnp.concatenate([down_w[0, at_w, own], down_w[0, at_w, other]], axis=1)
        hidden = contract_cols(held[...], weights)
        gate_pre[:, at_w] = (hidden * gate_f[:, at_w].astype(jnp.float32)).astype(gate_pre.dtype)
        up_pre[:, at_w] = (hidden * up_f[:, at_w].astype(jnp.float32)).astype(up_pre.dtype)

    def step(i, carry):
        piece(pl.multiple_of(i * 2 * LANES, 2 * LANES), 2 * LANES)
        return carry

    steps = count // (2 * LANES)
    lax.fori_loop(0, steps, step, 0)
    if count % (2 * LANES):
        piece(steps * 2 * LANES, count % (2 * LANES))


def held_block(k, refs, side_refs):
    if k == 0:
        return (refs[0][...], side_refs[0][...])
    rows = refs[0].shape[0]
    at = slice((k - 1) * rows, k * rows)
    return (refs[1][at, :], side_refs[1][at, :])


def act_kernel(columns, near_w, far_w, near_side_w, far_side_w, kept, given):
    blocks, rows, _ = columns.shape
    planes = blocks // 2
    plane = lax.axis_index("far")
    side = lax.axis_index("side")
    total = jnp.zeros((rows, near_w.shape[1]), jnp.float32)
    for k in range(planes):
        r = lax.rem(plane + planes - k, planes)
        here, beside = held_block(k, (near_w, far_w), (near_side_w, far_side_w))
        total = total + dotted(columns[2 * r + side], here)
        total = total + dotted(columns[2 * r + 1 - side], beside)
    kept[...] = total[: rows // 2]
    given[...] = total[rows // 2 :].astype(given.dtype)


def proj_kernel(columns, near, far, near_side, far_side, kept, given, total):
    planes = columns.shape[0] // 2
    plane = lax.axis_index("far")
    side = lax.axis_index("side")
    pair = lax.axis_index("pair")
    out = kept.shape[0]
    value = jnp.zeros(total.shape, jnp.float32)
    for k in range(planes):
        r = lax.rem(plane + planes - k, planes)
        here, beside = held_block(k, (near, far), (near_side, far_side))
        value = value + contract_rows(columns[2 * r + side], here)
        value = value + contract_rows(columns[2 * r + 1 - side], beside)
    total[...] = value
    kept[...] = total[pl.ds(pl.multiple_of(pair * out, out), out), :]
    given[...] = total[pl.ds(pl.multiple_of((1 - pair) * out, out), out), :].astype(given.dtype)


def back_kernel(part, gate_pre, up_pre, gate_w, up_w, kept, given):
    rows, half = kept.shape
    core = lax.axis_index("tp")
    at = pl.ds(part * rows, rows)
    block = 2 * LANES

    for out, place in ((given, 1 - core), (kept, core)):

        def step(i, carry, out=out, place=place):
            from_w = pl.ds(pl.multiple_of(place * half + i * block, block), block)
            value = contract_cols(gate_pre[at, :], gate_w[0, from_w, :]) + contract_cols(
                up_pre[at, :], up_w[0, from_w, :]
            )
            out[:, pl.ds(pl.multiple_of(i * block, block), block)] = value.astype(out.dtype)
            return carry

        lax.fori_loop(0, half // block, step, 0)


def grads_kernel(core_ref, *refs):
    mids, cots = (refs[:8], refs[8:16])
    act, gate_pre, up_pre, gate_ref, up_ref, down_ref = refs[16:]

    def fill(mids, cots):
        both = jnp.concatenate([piece[...] for piece in mids], axis=0)
        gate_ref[0] = contract_rows(both, gate_pre[...]).astype(gate_ref.dtype)
        up_ref[0] = contract_rows(both, up_pre[...]).astype(up_ref.dtype)
        both = jnp.concatenate([piece[...] for piece in cots], axis=0)
        down_ref[0] = contract_rows(act[...], both).astype(down_ref.dtype)

    @pl.when(pl.program_id(0) == 0)
    def _():
        fill(mids[:4], cots[:4])

    @pl.when(pl.program_id(0) != 0)
    def _():
        fill(mids[4:], cots[4:])


def weight_grads(core, mids, cots, act, gate_pre, up_pre):
    half = mids[0].shape[1]
    rows, hidden = act.shape
    block = 2 * LANES
    steps = half // block

    def piece(number, array):
        turn = number // 4

        def at(h, i, c):
            return (0, jnp.where(h == turn, i, (steps - 1) * (1 - turn)))

        return pl.BlockSpec((array.shape[0], block), at)

    def full(array):
        return pl.BlockSpec(array.shape, lambda h, i, c: (0, 0))

    spread = [piece(n, array) for n, array in enumerate(mids)]

    def out_rows(h, i, c):
        return (0, (h ^ c[0]) * steps + i, 0)

    def out_cols(h, i, c):
        return (0, 0, (h ^ c[0]) * steps + i)

    return pl.pallas_call(
        grads_kernel,
        grid_spec=pltpu.PrefetchScalarGridSpec(
            num_scalar_prefetch=1,
            grid=(2, steps),
            in_specs=[*spread, *spread, full(act), full(gate_pre), full(up_pre)],
            out_specs=[
                pl.BlockSpec((1, block, hidden), out_rows),
                pl.BlockSpec((1, block, hidden), out_rows),
                pl.BlockSpec((1, hidden, block), out_cols),
            ],
        ),
        out_shape=[
            jax.ShapeDtypeStruct((1, 2 * half, hidden), jnp.bfloat16),
            jax.ShapeDtypeStruct((1, 2 * half, hidden), jnp.bfloat16),
            jax.ShapeDtypeStruct((1, hidden, 2 * half), jnp.bfloat16),
        ],
        cost_estimate=pl.CostEstimate(
            flops=12 * rows * half * hidden, bytes_accessed=12 * half * hidden, transcendentals=0
        ),
        compiler_params=pltpu.CompilerParams(
            vmem_limit_bytes=40 << 20, dimension_semantics=("arbitrary", "arbitrary")
        ),
    )(core.reshape(1).astype(jnp.int32), *mids, *cots, act, gate_pre, up_pre)


def on_device(
    conv_out,
    ln_gain,
    taps,
    proj_weight,
    stream_mid,
    out_grad,
    routes,
    route_probs,
    gate_slabs,
    up_slabs,
    down_slabs,
):
    tok_rows, half = conv_out.shape
    width = half * lax.axis_size("tp")
    planes = lax.axis_size("far")
    experts = 2 * planes
    capacity = 3 * tok_rows // experts
    out_rows = proj_weight.shape[0]
    core = lax.axis_index("tp")
    plane = lax.axis_index("far")
    side = lax.axis_index("side")
    pair = lax.axis_index("pair")
    wide = planes * capacity
    hops = range(1, planes)

    info = jnp.concatenate([routes.astype(jnp.float32).T, route_probs.T], axis=0)
    beside_info = swapped(info, "side")
    beside_mid = swapped(stream_mid, "side")
    beside_grad = swapped(out_grad, "side")

    values = conv_out.astype(jnp.float32)
    sums = (jnp.sum(values, axis=1), jnp.sum(values * values, axis=1))
    row_total, row_squares = lax.psum(sums, "tp")
    row_mean = row_total[:, None] / width
    row_var = row_squares[:, None] / width - row_mean * row_mean
    inv_std = lax.rsqrt(row_var + 1e-06)
    normed = (values - row_mean) * inv_std
    scaled_z = normed * ln_gain[None, :]
    z_sig = jax.nn.sigmoid(scaled_z)
    activated = (scaled_z * z_sig).astype(jnp.bfloat16)

    targets = 2 * ((plane + jnp.arange(planes)) % planes) + side
    own_table, own_weights = slot_columns(info, targets, capacity)
    beside_table, beside_weights = slot_columns(beside_info, targets, capacity)

    def by_target(near, far):
        near, far = (
            block.astype(jnp.bfloat16).reshape(planes, capacity, half) for block in (near, far)
        )
        return [jnp.stack([near[k], far[k]]) for k in range(planes)]

    mid_slots = by_target(
        contract_rows(own_table, stream_mid), contract_rows(beside_table, beside_mid)
    )
    grad_slots = by_target(
        contract_rows(own_table, out_grad) * own_weights[:, None],
        contract_rows(beside_table, beside_grad) * beside_weights[:, None],
    )
    near_rows = 2 * capacity
    mid_far = [shifted(mid_slots[k], k) for k in hops]
    mid_near = mid_slots[0].reshape(near_rows, half)
    mid_near_pair = swapped(mid_near, "pair")
    mid_far, grad_slots, activated = fence((mid_far, grad_slots, activated))
    mid_mine = jnp.stack(mid_far).reshape(-1, half)
    mid_pair = swapped(mid_mine, "pair")
    grad_far = [shifted(grad_slots[k], k) for k in hops]
    grad_near = grad_slots[0].reshape(near_rows, half)
    grad_near_pair = swapped(grad_near, "pair")
    mid_pair, grad_far, grad_near_pair = fence((mid_pair, grad_far, grad_near_pair))
    proj_near_side = swapped(proj_weight, "side")
    act_near_side = swapped(activated, "side")
    grad_mine = jnp.stack(grad_far).reshape(-1, half)
    grad_pair = swapped(grad_mine, "pair")
    proj_far = [shifted(proj_weight, k) for k in hops]
    act_far = [shifted(activated, k) for k in hops]

    def pieces(*own):
        return (*own, *(swapped(p, "tp") for p in own))

    mids = pieces(mid_near, mid_mine, mid_near_pair, mid_pair)
    cots = pieces(grad_near, grad_mine, grad_near_pair, grad_pair)
    slots, hidden = (4 * wide, gate_slabs.shape[2])
    held = jax.ShapeDtypeStruct((slots, hidden), jnp.bfloat16)
    flops = 2 * slots * width * hidden
    hidden_act, gate_f, up_f = in_vmem(
        hidden_kernel,
        (held, held, held),
        2 * flops,
        (*mids, gate_slabs, up_slabs),
        (((slots, width), jnp.bfloat16),),
    )
    gate_pre, up_pre = in_vmem(
        pre_kernel,
        (held, held),
        flops,
        (*cots, down_slabs, gate_f, up_f),
        (((slots, width), jnp.bfloat16),),
    )
    summed = []
    for part in (1, 0):
        one = jax.ShapeDtypeStruct((2 * wide, half), jnp.bfloat16)
        kept, given = in_vmem(
            functools.partial(back_kernel, part),
            (one, one),
            flops,
            (gate_pre, up_pre, gate_slabs, up_slabs),
        )
        given = swapped(given, "tp")
        summed.append(kept.astype(jnp.float32) + given.astype(jnp.float32))
    proj_rest = jnp.concatenate(proj_far, axis=0)
    proj_side = swapped(proj_rest, "side")
    act_rest = jnp.concatenate(act_far, axis=0)
    act_side = swapped(act_rest, "side")
    moving = summed[0].astype(jnp.bfloat16)
    across = swapped(moving[near_rows:], "pair")
    across_near = swapped(moving[:near_rows], "pair")
    both = (summed[1][near_rows:] + across.astype(jnp.float32)).astype(jnp.bfloat16)
    both = both.reshape(planes - 1, 2, capacity, half)
    back_far = [shifted(both[k - 1], -k) for k in hops]
    back_near = (summed[1][:near_rows] + across_near.astype(jnp.float32)).astype(jnp.bfloat16)
    back = jnp.stack([back_near.reshape(2, capacity, half), *back_far])
    for_beside = jnp.dot(
        beside_table, back[:, 1].reshape(wide, half), preferred_element_type=jnp.float32
    ).astype(jnp.bfloat16)
    for_own = jnp.dot(
        own_table, back[:, 0].reshape(wide, half), preferred_element_type=jnp.float32
    )
    from_beside = swapped(for_beside, "side")
    grad_stream = (
        out_grad.astype(jnp.float32) + for_own + from_beside.astype(jnp.float32)
    ).astype(jnp.bfloat16)

    grad_gate, grad_up, grad_down = weight_grads(
        core, mids, cots, hidden_act, gate_pre, up_pre
    )

    blocks = half // (2 * out_rows)
    by_place = grad_stream.reshape(tok_rows, blocks, 2 * out_rows).transpose(1, 0, 2)
    by_pair = grad_stream.reshape(tok_rows, blocks, 2, out_rows).transpose(2, 1, 0, 3)
    stream_met = swapped(chosen(pair, by_pair[1], by_pair[0]), "pair")
    whole_stream = lax.all_gather(by_place, "tp", axis=0, tiled=True)
    columns = lax.all_to_all(whole_stream, ("far", "side"), split_axis=0, concat_axis=0, tiled=True)
    shared = jnp.concatenate([chosen(pair, by_pair[0], by_pair[1]), stream_met], axis=1)
    shared = lax.all_gather(shared, "tp", axis=0, tiled=True)
    act_kept, act_given = in_vmem(
        act_kernel,
        (
            jax.ShapeDtypeStruct((tok_rows, half), jnp.float32),
            jax.ShapeDtypeStruct((tok_rows, half), jnp.bfloat16),
        ),
        2 * tok_rows * width * half,
        (shared, proj_weight, proj_rest, proj_near_side, proj_side),
        limit=24,
    )
    act_met = swapped(act_given, "pair")
    grad_act = act_kept + act_met.astype(jnp.float32)
    grad_normed = grad_act * z_sig * (1.0 + scaled_z * (1.0 - z_sig)) * ln_gain[None, :]
    first_sum, second_sum = lax.psum(
        (jnp.sum(grad_normed, axis=1), jnp.sum(grad_normed * normed, axis=1)), "tp"
    )
    grad_conv = (
        inv_std * (grad_normed - first_sum[:, None] / width - normed * second_sum[:, None] / width)
    ).astype(jnp.bfloat16)
    reach_rows = taps.shape[0] - 1
    following = passed_along(grad_conv[:reach_rows], -1)
    extended = jnp.concatenate([grad_conv, following], axis=0).astype(jnp.float32)
    tap_values = taps.astype(jnp.float32)
    grad_input = jnp.zeros((tok_rows, grad_conv.shape[1]), jnp.float32)
    for offset in range(taps.shape[0]):
        grad_input = grad_input + tap_values[offset][None, :] * extended[offset : offset + tok_rows]

    proj_kept, proj_given = in_vmem(
        proj_kernel,
        (
            jax.ShapeDtypeStruct((out_rows, half), jnp.float32),
            jax.ShapeDtypeStruct((out_rows, half), jnp.bfloat16),
        ),
        2 * tok_rows * width * half,
        (columns, activated, act_rest, act_near_side, act_side),
        (((2 * out_rows, half), jnp.float32),),
    )
    proj_met = swapped(proj_given, "pair")
    grad_proj = proj_kept + proj_met.astype(jnp.float32)
    return (
        grad_input.astype(jnp.bfloat16),
        grad_proj,
        grad_gate,
        grad_up,
        grad_down,
    )


def solution(mesh):
    places, cores = mesh.devices.shape
    split = Mesh(mesh.devices.reshape(places // 4, 2, 2, cores), (*SP, "tp"))
    return jax.shard_map(
        on_device,
        mesh=split,
        in_specs=(
            P(SP, "tp"),
            P("tp"),
            P(None, "tp"),
            P(SP, "tp"),
            P(SP, "tp"),
            P(SP, "tp"),
            P(SP, None),
            P(SP, None),
            P(SP, None, "tp"),
            P(SP, None, "tp"),
            P(SP, "tp", None),
        ),
        out_specs=(
            P(SP, "tp"),
            P(SP, "tp"),
            P(SP, None, "tp"),
            P(SP, None, "tp"),
            P(SP, "tp", None),
        ),
        check_vma=False,
    )
```

```python
import functools

import jax
import jax.numpy as jnp
from jax import lax
from jax.experimental import pallas as pl
from jax.experimental.pallas import tpu as pltpu
from jax.sharding import Mesh
from jax.sharding import PartitionSpec as P


SP = ("far", "side", "pair")
fence = lax.optimization_barrier


def swapped(value, axis):
    return lax.ppermute(value, axis, [(0, 1), (1, 0)])


def shifted(value, steps):
    count = lax.axis_size("far")
    return lax.ppermute(value, "far", [(s, (s + steps) % count) for s in range(count)])


def passed_along(value, steps):
    count = lax.axis_size(SP)
    first, last = (max(0, -steps), min(count, count - steps))
    return lax.ppermute(value, SP, [(source, source + steps) for source in range(first, last)])


def chosen(bit, low, high):
    return jnp.where(bit == 0, low, high)


def slot_columns(info, targets, capacity):
    rows = info.shape[1]
    routes = info[0:2]
    probs = info[2:4]
    wide = targets.shape[0] * capacity
    earlier = (jnp.arange(rows)[:, None] > jnp.arange(rows)[None, :]).astype(jnp.bfloat16)
    target_of = jnp.repeat(targets, capacity).astype(jnp.float32)
    slot_of = (jnp.arange(wide) % capacity).astype(jnp.float32)
    first = routes[0][:, None] == target_of[None, :]
    second = routes[1][:, None] == target_of[None, :]
    named = (first | second).astype(jnp.bfloat16)
    before = jnp.dot(earlier, named, preferred_element_type=jnp.float32)
    here = before == slot_of[None, :]
    first, second = (first & here, second & here)
    weights = jnp.sum(
        jnp.where(first, probs[0][:, None], 0.0) + jnp.where(second, probs[1][:, None], 0.0),
        axis=0,
    )
    return ((first | second).astype(jnp.bfloat16), weights)


def contract_rows(left, right):
    return lax.dot_general(
        left, right, (((0,), (0,)), ((), ())), preferred_element_type=jnp.float32
    )


def contract_cols(left, right):
    return lax.dot_general(
        left, right, (((1,), (1,)), ((), ())), preferred_element_type=jnp.float32
    )


def own_and_other(half):
    core = lax.axis_index("tp")
    own = pl.ds(pl.multiple_of(core * half, half), half)
    other = pl.ds(pl.multiple_of((1 - core) * half, half), half)
    return (own, other)


def dotted(left, right):
    return jnp.dot(left, right, preferred_element_type=jnp.float32)


def in_vmem(kernel, shapes, flops, arrays, scratch=(), limit=24):
    return pl.pallas_call(
        kernel,
        out_shape=shapes,
        in_specs=[pl.BlockSpec(memory_space=pltpu.VMEM)] * len(arrays),
        out_specs=jax.tree.map(lambda _: pl.BlockSpec(memory_space=pltpu.VMEM), shapes),
        scratch_shapes=[pltpu.VMEM(shape, dtype) for shape, dtype in scratch],
        cost_estimate=pl.CostEstimate(
            flops=flops, bytes_accessed=sum(a.size * 2 for a in arrays), transcendentals=0
        ),
        compiler_params=pltpu.CompilerParams(vmem_limit_bytes=limit << 20),
    )(*arrays)


LANES = 128


def gathered(pieces, held):
    half = held.shape[1] // 2
    count = len(pieces) // 2
    for column, group in enumerate((pieces[:count], pieces[count:])):
        start = 0
        for piece in group:
            rows = piece.shape[0]
            held[start : start + rows, column * half : (column + 1) * half] = piece[...]
            start += rows


def hidden_kernel(*refs):
    pieces = refs[:8]
    gate_w, up_w, act_ref, gate_f, up_f, held = refs[8:]
    own, other = own_and_other(held.shape[1] // 2)
    gathered(pieces, held)

    def step(i, carry):
        cols = pl.ds(pl.multiple_of(i * LANES, LANES), LANES)
        own_w = jnp.concatenate([gate_w[0, own, cols], up_w[0, own, cols]], axis=1)
        oth_w = jnp.concatenate([gate_w[0, other, cols], up_w[0, other, cols]], axis=1)
        both = dotted(held[...], jnp.concatenate([own_w, oth_w], axis=0))
        gate, up = (both[:, :LANES], both[:, LANES:])
        sig = jax.nn.sigmoid(gate)
        silu = gate * sig
        act_ref[:, cols] = (silu * up).astype(act_ref.dtype)
        gate_f[:, cols] = (up * sig * (1.0 + gate * (1.0 - sig))).astype(gate_f.dtype)
        up_f[:, cols] = silu.astype(up_f.dtype)
        return carry

    lax.fori_loop(0, gate_w.shape[2] // LANES, step, 0)


def pre_kernel(*refs):
    pieces = refs[:8]
    down_w, gate_f, up_f, gate_pre, up_pre, held = refs[8:]
    own, other = own_and_other(held.shape[1] // 2)
    count = down_w.shape[1]
    gathered(pieces, held)

    def piece(start, size):
        at_w = pl.ds(start, size)
        weights = jnp.concatenate([down_w[0, at_w, own], down_w[0, at_w, other]], axis=1)
        hidden = contract_cols(held[...], weights)
        gate_pre[:, at_w] = (hidden * gate_f[:, at_w].astype(jnp.float32)).astype(gate_pre.dtype)
        up_pre[:, at_w] = (hidden * up_f[:, at_w].astype(jnp.float32)).astype(up_pre.dtype)

    def step(i, carry):
        piece(pl.multiple_of(i * 2 * LANES, 2 * LANES), 2 * LANES)
        return carry

    steps = count // (2 * LANES)
    lax.fori_loop(0, steps, step, 0)
    if count % (2 * LANES):
        piece(steps * 2 * LANES, count % (2 * LANES))


def block_of(k, stacks, refs):
    for stack, ref in zip(stacks, refs, strict=True):
        if k in stack:
            rows = ref.shape[0] // len(stack)
            at = stack.index(k) * rows
            return ref[at : at + rows, :]
    raise ValueError(k)


def act_kernel(stacks, kept_cols, met_cols, *refs):
    weights, (kept, given) = (refs[:-2], refs[-2:])
    count = len(stacks)
    blocks, rows, _ = kept_cols.shape
    planes = blocks // 2
    plane = lax.axis_index("far")
    side = lax.axis_index("side")
    total = jnp.zeros((2 * rows, kept.shape[1]), jnp.float32)
    for k in range(planes):
        r = lax.rem(plane + planes - k, planes)
        for at, held in ((2 * r + side, weights[:count]), (2 * r + 1 - side, weights[count:])):
            both = jnp.concatenate([kept_cols[at], met_cols[at]], axis=0)
            total = total + dotted(both, block_of(k, stacks, held))
    kept[...] = total[:rows]
    given[...] = total[rows:].astype(given.dtype)


def proj_kernel(stacks, columns, *refs):
    acts, (kept, given, total) = (refs[:-3], refs[-3:])
    count = len(stacks)
    planes = columns.shape[0] // 2
    plane = lax.axis_index("far")
    side = lax.axis_index("side")
    pair = lax.axis_index("pair")
    out = kept.shape[0]
    value = jnp.zeros(total.shape, jnp.float32)
    for k in range(planes):
        r = lax.rem(plane + planes - k, planes)
        for at, held in ((2 * r + side, acts[:count]), (2 * r + 1 - side, acts[count:])):
            value = value + contract_rows(columns[at], block_of(k, stacks, held))
    total[...] = value
    kept[...] = total[pl.ds(pl.multiple_of(pair * out, out), out), :]
    given[...] = total[pl.ds(pl.multiple_of((1 - pair) * out, out), out), :].astype(given.dtype)


def back_kernel(part, gate_pre, up_pre, gate_w, up_w, kept, given):
    rows, half = kept.shape
    core = lax.axis_index("tp")
    at = pl.ds(part * rows, rows)
    block = 2 * LANES

    for out, place in ((given, 1 - core), (kept, core)):

        def step(i, carry, out=out, place=place):
            from_w = pl.ds(pl.multiple_of(place * half + i * block, block), block)
            value = contract_cols(gate_pre[at, :], gate_w[0, from_w, :]) + contract_cols(
                up_pre[at, :], up_w[0, from_w, :]
            )
            out[:, pl.ds(pl.multiple_of(i * block, block), block)] = value.astype(out.dtype)
            return carry

        lax.fori_loop(0, half // block, step, 0)


def grads_kernel(core_ref, *refs):
    mids, cots = (refs[:8], refs[8:16])
    act, gate_pre, up_pre, gate_ref, up_ref, down_ref = refs[16:]

    def fill(mids, cots):
        both = jnp.concatenate([piece[...] for piece in mids], axis=0)
        gate_ref[0] = contract_rows(both, gate_pre[...]).astype(gate_ref.dtype)
        up_ref[0] = contract_rows(both, up_pre[...]).astype(up_ref.dtype)
        both = jnp.concatenate([piece[...] for piece in cots], axis=0)
        down_ref[0] = contract_rows(act[...], both).astype(down_ref.dtype)

    @pl.when(pl.program_id(0) == 0)
    def _():
        fill(mids[:4], cots[:4])

    @pl.when(pl.program_id(0) != 0)
    def _():
        fill(mids[4:], cots[4:])


def weight_grads(core, mids, cots, act, gate_pre, up_pre):
    half = mids[0].shape[1]
    rows, hidden = act.shape
    block = 2 * LANES
    steps = half // block

    def piece(number, array):
        turn = number // 4

        def at(h, i, c):
            return (0, jnp.where(h == turn, i, (steps - 1) * (1 - turn)))

        return pl.BlockSpec((array.shape[0], block), at)

    def full(array):
        return pl.BlockSpec(array.shape, lambda h, i, c: (0, 0))

    spread = [piece(n, array) for n, array in enumerate(mids)]

    def out_rows(h, i, c):
        return (0, (h ^ c[0]) * steps + i, 0)

    def out_cols(h, i, c):
        return (0, 0, (h ^ c[0]) * steps + i)

    return pl.pallas_call(
        grads_kernel,
        grid_spec=pltpu.PrefetchScalarGridSpec(
            num_scalar_prefetch=1,
            grid=(2, steps),
            in_specs=[*spread, *spread, full(act), full(gate_pre), full(up_pre)],
            out_specs=[
                pl.BlockSpec((1, block, hidden), out_rows),
                pl.BlockSpec((1, block, hidden), out_rows),
                pl.BlockSpec((1, hidden, block), out_cols),
            ],
        ),
        out_shape=[
            jax.ShapeDtypeStruct((1, 2 * half, hidden), jnp.bfloat16),
            jax.ShapeDtypeStruct((1, 2 * half, hidden), jnp.bfloat16),
            jax.ShapeDtypeStruct((1, hidden, 2 * half), jnp.bfloat16),
        ],
        cost_estimate=pl.CostEstimate(
            flops=12 * rows * half * hidden, bytes_accessed=12 * half * hidden, transcendentals=0
        ),
        compiler_params=pltpu.CompilerParams(
            vmem_limit_bytes=40 << 20, dimension_semantics=("arbitrary", "arbitrary")
        ),
    )(core.reshape(1).astype(jnp.int32), *mids, *cots, act, gate_pre, up_pre)


def on_device(
    conv_out,
    ln_gain,
    taps,
    proj_weight,
    stream_mid,
    out_grad,
    routes,
    route_probs,
    gate_slabs,
    up_slabs,
    down_slabs,
):
    tok_rows, half = conv_out.shape
    width = half * lax.axis_size("tp")
    planes = lax.axis_size("far")
    experts = 2 * planes
    capacity = 3 * tok_rows // experts
    out_rows = proj_weight.shape[0]
    core = lax.axis_index("tp")
    plane = lax.axis_index("far")
    side = lax.axis_index("side")
    pair = lax.axis_index("pair")
    wide = planes * capacity
    hops = range(1, planes)

    info = jnp.concatenate([routes.astype(jnp.float32).T, route_probs.T], axis=0)
    beside_info = swapped(info, "side")
    beside_mid = swapped(stream_mid, "side")
    beside_grad = swapped(out_grad, "side")

    values = conv_out.astype(jnp.float32)
    sums = (jnp.sum(values, axis=1), jnp.sum(values * values, axis=1))
    row_total, row_squares = lax.psum(sums, "tp")
    row_mean = row_total[:, None] / width
    row_var = row_squares[:, None] / width - row_mean * row_mean
    inv_std = lax.rsqrt(row_var + 1e-06)
    normed = (values - row_mean) * inv_std
    scaled_z = normed * ln_gain[None, :]
    z_sig = jax.nn.sigmoid(scaled_z)
    activated = (scaled_z * z_sig).astype(jnp.bfloat16)

    targets = 2 * ((plane + jnp.arange(planes)) % planes) + side
    own_table, own_weights = slot_columns(info, targets, capacity)
    beside_table, beside_weights = slot_columns(beside_info, targets, capacity)

    def by_target(near, far):
        near, far = (
            block.astype(jnp.bfloat16).reshape(planes, capacity, half) for block in (near, far)
        )
        return [jnp.stack([near[k], far[k]]) for k in range(planes)]

    mid_slots = by_target(
        contract_rows(own_table, stream_mid), contract_rows(beside_table, beside_mid)
    )
    grad_slots = by_target(
        contract_rows(own_table, out_grad) * own_weights[:, None],
        contract_rows(beside_table, beside_grad) * beside_weights[:, None],
    )
    near_rows = 2 * capacity
    mid_far = [shifted(mid_slots[k], k) for k in hops]
    mid_near = mid_slots[0].reshape(near_rows, half)
    mid_near_pair = swapped(mid_near, "pair")
    mid_far, grad_slots, activated = fence((mid_far, grad_slots, activated))
    mid_mine = jnp.stack(mid_far).reshape(-1, half)
    mid_pair = swapped(mid_mine, "pair")
    grad_far = [shifted(grad_slots[k], k) for k in hops]
    grad_near = grad_slots[0].reshape(near_rows, half)
    grad_near_pair = swapped(grad_near, "pair")
    mid_pair, grad_far, grad_near_pair = fence((mid_pair, grad_far, grad_near_pair))
    proj_near_side = swapped(proj_weight, "side")
    grad_mine = jnp.stack(grad_far).reshape(-1, half)
    grad_pair = swapped(grad_mine, "pair")
    proj_far = [shifted(proj_weight, k) for k in hops]
    act_far = [shifted(activated, k) for k in hops]

    def pieces(*own):
        return (*own, *(swapped(p, "tp") for p in own))

    mids = pieces(mid_near, mid_mine, mid_near_pair, mid_pair)
    cots = pieces(grad_near, grad_mine, grad_near_pair, grad_pair)
    slots, hidden = (4 * wide, gate_slabs.shape[2])
    held = jax.ShapeDtypeStruct((slots, hidden), jnp.bfloat16)
    flops = 2 * slots * width * hidden
    hidden_act, gate_f, up_f = in_vmem(
        hidden_kernel,
        (held, held, held),
        2 * flops,
        (*mids, gate_slabs, up_slabs),
        (((slots, width), jnp.bfloat16),),
    )
    gate_pre, up_pre = in_vmem(
        pre_kernel,
        (held, held),
        flops,
        (*cots, down_slabs, gate_f, up_f),
        (((slots, width), jnp.bfloat16),),
    )
    summed = []
    for part in (1, 0):
        one = jax.ShapeDtypeStruct((2 * wide, half), jnp.bfloat16)
        kept, given = in_vmem(
            functools.partial(back_kernel, part),
            (one, one),
            flops,
            (gate_pre, up_pre, gate_slabs, up_slabs),
        )
        given = swapped(given, "tp")
        summed.append(kept.astype(jnp.float32) + given.astype(jnp.float32))
    proj_rest = jnp.concatenate(proj_far, axis=0)
    proj_side = swapped(proj_rest, "side")
    proj_stacks = ((0,), tuple(hops))
    late = planes // 2
    first = tuple(k for k in range(planes) if k != late)
    act_stacks = (first, (late,))
    act_all = [activated, *act_far]
    act_first = jnp.concatenate([act_all[k] for k in first], axis=0)
    act_first_side = swapped(act_first, "side")
    act_late = act_all[late]
    act_late_side = swapped(act_late, "side")
    moving = summed[0].astype(jnp.bfloat16)
    across = swapped(moving[near_rows:], "pair")
    across_near = swapped(moving[:near_rows], "pair")
    both = (summed[1][near_rows:] + across.astype(jnp.float32)).astype(jnp.bfloat16)
    both = both.reshape(planes - 1, 2, capacity, half)
    back_far = [shifted(both[k - 1], -k) for k in hops]
    back_near = (summed[1][:near_rows] + across_near.astype(jnp.float32)).astype(jnp.bfloat16)
    back = jnp.stack([back_near.reshape(2, capacity, half), *back_far])
    for_beside = jnp.dot(
        beside_table, back[:, 1].reshape(wide, half), preferred_element_type=jnp.float32
    ).astype(jnp.bfloat16)
    for_own = out_grad.astype(jnp.float32) + jnp.dot(
        own_table, back[:, 0].reshape(wide, half), preferred_element_type=jnp.float32
    )
    for_own = fence(for_own)
    from_beside = swapped(for_beside, "side")
    grad_stream = (for_own + from_beside.astype(jnp.float32)).astype(jnp.bfloat16)

    grad_gate, grad_up, grad_down = weight_grads(
        core, mids, cots, hidden_act, gate_pre, up_pre
    )

    blocks = half // (2 * out_rows)
    by_place = grad_stream.reshape(tok_rows, blocks, 2 * out_rows).transpose(1, 0, 2)
    by_pair = grad_stream.reshape(tok_rows, blocks, 2, out_rows).transpose(2, 1, 0, 3)
    stream_met = swapped(chosen(pair, by_pair[1], by_pair[0]), "pair")
    whole_stream = lax.all_gather(by_place, "tp", axis=0, tiled=True)
    columns = lax.all_to_all(whole_stream, ("far", "side"), split_axis=0, concat_axis=0, tiled=True)
    kept_cols = lax.all_gather(
        chosen(pair, by_pair[0], by_pair[1]), "tp", axis=0, tiled=True
    )
    met_cols = lax.all_gather(stream_met, "tp", axis=0, tiled=True)
    act_kept, act_given = in_vmem(
        functools.partial(act_kernel, proj_stacks),
        (
            jax.ShapeDtypeStruct((tok_rows, half), jnp.float32),
            jax.ShapeDtypeStruct((tok_rows, half), jnp.bfloat16),
        ),
        2 * tok_rows * width * half,
        (kept_cols, met_cols, proj_weight, proj_rest, proj_near_side, proj_side),
        limit=24,
    )
    act_met = swapped(act_given, "pair")
    grad_act = act_kept + act_met.astype(jnp.float32)
    grad_normed = grad_act * z_sig * (1.0 + scaled_z * (1.0 - z_sig)) * ln_gain[None, :]
    first_sum, second_sum = lax.psum(
        (jnp.sum(grad_normed, axis=1), jnp.sum(grad_normed * normed, axis=1)), "tp"
    )
    grad_conv = (
        inv_std * (grad_normed - first_sum[:, None] / width - normed * second_sum[:, None] / width)
    ).astype(jnp.bfloat16)
    reach_rows = taps.shape[0] - 1
    following = passed_along(grad_conv[:reach_rows], -1)
    extended = jnp.concatenate([grad_conv, following], axis=0).astype(jnp.float32)
    tap_values = taps.astype(jnp.float32)
    grad_input = jnp.zeros((tok_rows, grad_conv.shape[1]), jnp.float32)
    for offset in range(taps.shape[0]):
        grad_input = grad_input + tap_values[offset][None, :] * extended[offset : offset + tok_rows]

    proj_kept, proj_given = in_vmem(
        functools.partial(proj_kernel, act_stacks),
        (
            jax.ShapeDtypeStruct((out_rows, half), jnp.float32),
            jax.ShapeDtypeStruct((out_rows, half), jnp.bfloat16),
        ),
        2 * tok_rows * width * half,
        (columns, act_first, act_late, act_first_side, act_late_side),
        (((2 * out_rows, half), jnp.float32),),
    )
    proj_met = swapped(proj_given, "pair")
    grad_proj = proj_kept + proj_met.astype(jnp.float32)
    return (
        grad_input.astype(jnp.bfloat16),
        grad_proj,
        grad_gate,
        grad_up,
        grad_down,
    )


def solution(mesh):
    places, cores = mesh.devices.shape
    split = Mesh(mesh.devices.reshape(places // 4, 2, 2, cores), (*SP, "tp"))
    return jax.shard_map(
        on_device,
        mesh=split,
        in_specs=(
            P(SP, "tp"),
            P("tp"),
            P(None, "tp"),
            P(SP, "tp"),
            P(SP, "tp"),
            P(SP, "tp"),
            P(SP, None),
            P(SP, None),
            P(SP, None, "tp"),
            P(SP, None, "tp"),
            P(SP, "tp", None),
        ),
        out_specs=(
            P(SP, "tp"),
            P(SP, "tp"),
            P(SP, None, "tp"),
            P(SP, None, "tp"),
            P(SP, "tp", None),
        ),
        check_vma=False,
    )
```
